32 devices in a mesh: fs: 8 (over z, y), tp: 4 (over x, core).
Axes of the slice: x: 2, y: 2, z: 4, core: 2. Of those that a mesh axis runs over, the one named last changes fastest.
Arguments:
- tokens: bfloat16 [8192, 2048], P('fs', 'tp'), may hold values from -6 to 6
- mixer_gain: float32 [2048], replicated, may hold values from 0.1 to 1.9
- conv_taps: bfloat16 [3, 1024], replicated, may hold values from -3.5 to 3.5
- outer_weight: bfloat16 [2048, 1024], P('fs', 'tp'), may hold values from -0.125 to 0.125
- inner_weight: bfloat16 [2048, 1024], P('fs', 'tp'), may hold values from -0.125 to 0.125
- value_weight: bfloat16 [2048, 1024], P('fs', 'tp'), may hold values from -0.125 to 0.125
- merge_weight: bfloat16 [1024, 2048], P('tp', 'fs'), may hold values from -0.25 to 0.25
- merge_gain: float32 [2048], replicated, may hold values from 0.1 to 1.9
- channel_gain: float32 [2048], replicated, may hold values from 0.1 to 1.9
- gate_weight: bfloat16 [2048, 5632], P('fs', 'tp'), may hold values from -0.125 to 0.125
- up_weight: bfloat16 [2048, 5632], P('fs', 'tp'), may hold values from -0.125 to 0.125
- down_weight: bfloat16 [5632, 2048], P('tp', 'fs'), may hold values from -0.109375 to 0.109375
- output_gain: float32 [2048], replicated, may hold values from 0.1 to 1.9
Outputs:
- layer_out: bfloat16 [8192, 2048], P('fs', 'tp')
The draws below stay inside these ranges and needn't reach their ends.
All inputs are finite; a program needn't handle non-finite values.
Results may differ from the reference program's by a relative error of at most 0.018.
Values may be sent and summed in bfloat16 or wider, within the bound.
A program may use at most 128 MiB of HBM per device.

```python
import jax
import jax.numpy as jnp
from jax import lax

D = 2048
HEADS = 8
HEAD_DIM = 128
TAPS = 3
FF = 5632
SEQ = 1024
CONV_WIDTH = 1024
TOKENS = 8192
N_FS = 8
N_TP = 4


def strengthened(array, key, source, target, shards_of, factor):
    def block_of(axis_at):
        return (jnp.arange(array.shape[axis_at]) // (array.shape[axis_at] // shards_of)).reshape((-1,) + (1,) * (array.ndim - 1 - axis_at))

    first = jax.random.permutation(key, shards_of)[block_of(target)]
    far = (block_of(target) + shards_of // 2) % shards_of
    return jnp.where((block_of(source) == first) | (block_of(source) == far), factor * array, array)


def block_scale(stream_key, extent, cuts, smallest, largest):
    level, own = 1.0, jax.random.fold_in(stream_key, 6)
    for position, blocks in cuts:
        heights = jnp.exp(jax.random.uniform(jax.random.fold_in(own, position), (blocks,), jnp.float32, smallest / len(cuts), largest / len(cuts)))
        level = level * jnp.repeat(heights, extent[position] // blocks).reshape([-1 if axis == position else 1 for axis in range(len(extent))])
    return level


def gaussian(stream_key, dims, scale, bound, pieces=(), held_as=jnp.bfloat16):
    entries = scale * jax.random.normal(stream_key, dims, jnp.float32)
    if pieces:
        entries = entries * block_scale(stream_key, dims, pieces, -0.22, 0.18)
    return jnp.clip(entries, -bound, bound).astype(held_as)


def heavy_noise(own_key, shape, width, bound, cuts, heavy, dtype=jnp.bfloat16):
    array = width * jax.random.normal(own_key, shape, jnp.float32)
    if cuts:
        array = array * block_scale(own_key, shape, cuts, -0.22, 0.18)
    return jnp.clip(strengthened(array, jax.random.fold_in(own_key, 3), *heavy), -bound, bound).astype(dtype)


def setup_inputs(seed: int = 0) -> dict:
    arg_keys = jax.random.split(jax.random.key(seed), 14)
    return {
        "tokens": gaussian(arg_keys[0], (TOKENS, D), 1.0, 6.0, ((0, 8), (1, 4))),
        "mixer_gain": jnp.clip(1.0 + 0.18 * jax.random.normal(arg_keys[1], (D,), jnp.float32), 0.1, 1.9),
        "conv_taps": gaussian(arg_keys[2], (TAPS, CONV_WIDTH), TAPS ** -0.5, 3.5),
        "outer_weight": gaussian(arg_keys[3], (D, CONV_WIDTH), D ** -0.5, 0.125, ((0, 8), (1, 4))),
        "inner_weight": gaussian(arg_keys[4], (D, CONV_WIDTH), D ** -0.5, 0.125, ((0, 8), (1, 4))),
        "value_weight": gaussian(arg_keys[5], (D, CONV_WIDTH), D ** -0.5, 0.125, ((0, 8), (1, 4))),
        "merge_weight": heavy_noise(arg_keys[6], (CONV_WIDTH, D), CONV_WIDTH ** -0.5, 0.25, ((0, 4), (1, 8)), (0, 1, 8, 2.0)),
        "merge_gain": jnp.clip(1.0 + 0.18 * jax.random.normal(arg_keys[7], (D,), jnp.float32), 0.1, 1.9),
        "channel_gain": jnp.clip(1.0 + 0.18 * jax.random.normal(arg_keys[8], (D,), jnp.float32), 0.1, 1.9),
        "gate_weight": gaussian(arg_keys[9], (D, FF), D ** -0.5, 0.125, ((0, 8), (1, 4))),
        "up_weight": gaussian(arg_keys[10], (D, FF), D ** -0.5, 0.125, ((0, 8), (1, 4))),
        "down_weight": heavy_noise(arg_keys[11], (FF, D), FF ** -0.5, 0.109375, ((0, 4), (1, 8)), (0, 1, 8, 2.0)),
        "output_gain": jnp.clip(1.0 + 0.18 * jax.random.normal(arg_keys[12], (D,), jnp.float32), 0.1, 1.9),
    }


EPS = 1e-06

def normalize(values):
    floats = values.astype(jnp.float32)
    return floats * lax.rsqrt(lax.optimization_barrier(jnp.mean(floats * floats, axis=-1, keepdims=True)) + EPS)

def causal_taps(signal, taps):
    length = signal.shape[0]
    padded = jnp.pad(signal, ((2, 0), (0, 0)))
    return taps[0] * padded[:length] + taps[1] * padded[1:length + 1] + taps[2] * padded[2:]

def blocked_sum(hidden, weight):
    length = hidden.shape[0]
    block_rows = hidden.shape[1] // N_TP
    left = hidden.astype(jnp.float32).reshape(length, N_TP, block_rows)
    right = weight.astype(jnp.float32).reshape(N_TP, block_rows, weight.shape[1])
    partials = jnp.einsum('sbc,bcd->bsd', left, right)
    rounded = lax.optimization_barrier(partials.astype(jnp.bfloat16)).astype(jnp.float32)
    return lax.optimization_barrier(jnp.sum(rounded, axis=0)).astype(jnp.bfloat16)

def reference(tokens, mixer_gain, conv_taps, outer_weight, inner_weight, value_weight, merge_weight, merge_gain, channel_gain, gate_weight, up_weight, down_weight, output_gain):
    taps_float = conv_taps.astype(jnp.float32)

    def one_sequence(rows):
        normed = (normalize(rows) * mixer_gain).astype(jnp.bfloat16)
        outer = jnp.dot(normed, outer_weight, preferred_element_type=jnp.float32)
        inner = jnp.dot(normed, inner_weight, preferred_element_type=jnp.float32)
        value = jnp.dot(normed, value_weight, preferred_element_type=jnp.float32)
        conv = causal_taps(inner * value, taps_float)
        gated = (outer * conv).reshape(rows.shape[0], HEADS, HEAD_DIM)
        mixed = normalize(gated).reshape(rows.shape[0], CONV_WIDTH).astype(jnp.bfloat16)
        merged = blocked_sum(mixed, merge_weight)
        first = (rows.astype(jnp.float32) + normalize(merged) * merge_gain).astype(jnp.bfloat16)
        normed2 = (normalize(first) * channel_gain).astype(jnp.bfloat16)
        gate = jnp.dot(normed2, gate_weight, preferred_element_type=jnp.float32)
        upward = jnp.dot(normed2, up_weight, preferred_element_type=jnp.float32)
        hidden = (jax.nn.silu(gate) * upward).astype(jnp.bfloat16)
        down = blocked_sum(hidden, down_weight)
        return (first.astype(jnp.float32) + normalize(down) * output_gain).astype(jnp.bfloat16)
    outputs = lax.map(one_sequence, tokens.reshape(N_FS, SEQ, D))
    return outputs.reshape(TOKENS, D)
```

```python
import jax
import jax.numpy as jnp
from jax import lax
from jax.experimental import pallas as pl
from jax.experimental.pallas import tpu as pltpu
from jax.sharding import PartitionSpec as P

HEAD_DIM = 128
EPS = 1e-06
MESH = pl.DeviceIdType.MESH
F32 = jnp.float32
BF16 = jnp.bfloat16
MIX, FEED, DOWN = (0, 1, 2, 3), (4, 5), (6, 7)


def layer_kernel(
    n, nt, tokens, mixer_gain, taps, outer_w, inner_w, value_w, merge_w, merge_gain,
    channel_gain, gate_w, up_w, down_w,
    down_out, first_out,
    toks, nrm, full_outer, full_inner, full_value, full_merge, full_gate, full_up, full_down,
    outer_s, sig, mixed, part, mrecv, msum, merged, hidden, drecv,
    ring_send, ring_recv, tok_send, tok_recv, rs_send, rs_recv, ag_send, ag_recv, dn_send, dn_recv,
):
    f, t = lax.axis_index("fs"), lax.axis_index("tp")
    half = n // 2
    odd = lax.rem(f, 2)
    pos = (1 - odd) * (f // 2) + odd * (n - 1 - f // 2)
    length, width = tokens.shape
    blk, channels = outer_w.shape
    cols = merge_w.shape[1]
    bps = n // nt
    depth = width * nt
    tile = min(256, length)
    tiles = length // tile

    def owner(p):
        q = lax.rem(p + 2 * n, n)
        high = q // half
        return (1 - high) * (2 * q) + high * (2 * (n - 1 - q) + 1)

    right, left = owner(pos + 1), owner(pos - 1)
    rowed = {0: (outer_w, full_outer), 1: (inner_w, full_inner), 2: (value_w, full_value),
             4: (gate_w, full_gate), 5: (up_w, full_up)}
    piece_m = channels // 2
    piece_d = down_w.shape[0] // 4

    def own_region(w, d):
        if w in rowed:
            return rowed[w][0].at[pl.ds(d * (blk // 2), blk // 2)]
        if w == 3:
            return merge_w.at[pl.ds(d * piece_m, piece_m)]
        return down_w.at[pl.ds((d * 2 + w - 6) * piece_d, piece_d)]

    def region(w, d, p):
        i = owner(p)
        if w in rowed:
            start = pl.multiple_of(i * blk + d * (blk // 2), blk // 2)
            return rowed[w][1].at[pl.ds(start, blk // 2)]
        if w == 3:
            return full_merge.at[i, pl.ds(d * piece_m, piece_m)]
        return full_down.at[i, pl.ds((d * 2 + w - 6) * piece_d, piece_d)]

    def ring_copy(w, d, s, first=False):
        p = pos - s if d == 0 else pos + s
        dst = region(w, d, p)
        return pltpu.make_async_remote_copy(
            src_ref=own_region(w, d) if first else dst,
            dst_ref=dst,
            send_sem=ring_send.at[d, w],
            recv_sem=ring_recv.at[d, w, s],
            device_id={"fs": right if d == 0 else left},
            device_id_type=MESH,
        )

    def ring_arrive(w, d, s):
        got = region(w, d, pos - 1 - s if d == 0 else pos + 1 + s)
        pltpu.make_async_remote_copy(
            src_ref=got, dst_ref=got, send_sem=ring_send.at[d, w],
            recv_sem=ring_recv.at[d, w, s],
            device_id={"fs": right if d == 0 else left}, device_id_type=MESH,
        ).wait_recv()

    def ring_open(ws):
        for w in ws:
            for d in (0, 1):
                ring_copy(w, d, 0, True).start()

    def pump(ws, s):
        for w in ws:
            for d in (0, 1):
                ring_arrive(w, d, s - 1)
                ring_copy(w, d, s - 1).wait_send()
                ring_copy(w, d, s).start()

    def pumps(ws, low, high):
        lax.fori_loop(low, high, lambda s, c: (pump(ws, s), c)[1], 0)

    def ring_close(ws):
        for w in ws:
            for d in (0, 1):
                ring_arrive(w, d, n - 2)
                ring_copy(w, d, n - 2).wait_send()

    def peer(o):
        return lax.rem(t + o, nt)

    def slab_copy(src, dst, send, recv, o):
        return pltpu.make_async_remote_copy(
            src_ref=src, dst_ref=dst, send_sem=send.at[o - 1], recv_sem=recv.at[o - 1],
            device_id={"tp": peer(o)}, device_id_type=MESH,
        )

    offsets = range(1, nt)

    barrier = pltpu.get_barrier_semaphore()
    for to in ({"fs": left}, {"fs": right}) + tuple({"tp": peer(o)} for o in offsets):
        pl.semaphore_signal(barrier, inc=1, device_id=to, device_id_type=MESH)
    pl.semaphore_wait(barrier, 2 + nt - 1)

    ring_open(MIX)
    for o in offsets:
        slab_copy(tokens, toks.at[t], tok_send, tok_recv, o).start()

    own_rows = pl.ds(pl.multiple_of(f * blk, blk), blk)
    for source, full in rowed.values():
        full[own_rows, :] = source[...]
    full_merge[f] = merge_w[...]
    full_down[f] = down_w[...]
    toks[t] = tokens[...]
    sig[pl.ds(0, 8), :] = jnp.zeros((8, channels), F32)

    pumps(MIX, 1, n - 1)
    ring_open(FEED)
    for o in offsets:
        slab = toks.at[lax.rem(t - o + nt, nt)]
        slab_copy(tokens, slab, tok_send, tok_recv, o).wait()

    def rows_of(i):
        return pl.ds(pl.multiple_of(i * tile, tile), tile)

    def norm_tile(i, c):
        rows = rows_of(i)
        squares = jnp.zeros((tile, 1), F32)
        for j in range(nt):
            x = toks[j, rows, :].astype(F32)
            squares += jnp.sum(x * x, axis=1, keepdims=True)
        factor = lax.rsqrt(squares / depth + EPS)
        for j in range(nt):
            x = toks[j, rows, :].astype(F32)
            nrm[rows, pl.ds(j * width, width)] = (x * factor * mixer_gain[j]).astype(BF16)
        return c

    lax.fori_loop(0, tiles, norm_tile, 0)
    ring_close(MIX)

    def project(i, c):
        rows = rows_of(i)
        x = nrm[rows, :]
        outer_s[rows, :] = jnp.dot(x, full_outer[...], preferred_element_type=F32)
        inner = jnp.dot(x, full_inner[...], preferred_element_type=F32)
        value = jnp.dot(x, full_value[...], preferred_element_type=F32)
        sig[pl.ds(pl.multiple_of(i * tile + 8, 8), tile), :] = inner * value
        return c

    lax.fori_loop(0, tiles, project, 0)
    for i in range(tiles):
        r = i * tile
        conv = (
            taps[0:1, :] * sig[r + 6 : r + 6 + tile, :]
            + taps[1:2, :] * sig[r + 7 : r + 7 + tile, :]
            + taps[2:3, :] * sig[r + 8 : r + 8 + tile, :]
        )
        gated = outer_s[r : r + tile, :] * conv
        for h in range(channels // HEAD_DIM):
            g = gated[:, h * HEAD_DIM : (h + 1) * HEAD_DIM]
            level = lax.rsqrt(jnp.mean(g * g, axis=1, keepdims=True) + EPS)
            mixed[r : r + tile, h * HEAD_DIM : (h + 1) * HEAD_DIM] = (g * level).astype(BF16)

    def merge_block(b, c):
        part[b] = jnp.dot(mixed[...], full_merge[b], preferred_element_type=F32).astype(BF16)
        return c

    lax.fori_loop(0, n, merge_block, 0)

    def part_slab(j):
        return part.at[pl.ds(j * bps, bps)]

    for o in offsets:
        slab_copy(part_slab(peer(o)), mrecv.at[o - 1], rs_send, rs_recv, o).start()
    cut = (2 * (n - 2) + 2) // 3
    pumps(FEED, 1, cut + 1)
    for o in offsets:
        slab_copy(part_slab(peer(o)), mrecv.at[o - 1], rs_send, rs_recv, o).wait()

    def add_tile(received, target):
        def body(i, c):
            rows = rows_of(i)
            for q in range(bps):
                total = part[t * bps + q, rows, :].astype(F32)
                for o in offsets:
                    total += received[o - 1, q, rows, :].astype(F32)
                target[rows, pl.ds(q * cols, cols)] = total.astype(BF16)
            return c

        lax.fori_loop(0, tiles, body, 0)

    add_tile(mrecv, msum)
    for o in offsets:
        slab_copy(msum, merged.at[t], ag_send, ag_recv, o).start()
    merged[t] = msum[...]
    pumps(FEED, cut + 1, n - 1)
    ring_open(DOWN)
    for o in offsets:
        slab = merged.at[lax.rem(t - o + nt, nt)]
        slab_copy(msum, slab, ag_send, ag_recv, o).wait()

    def first_tile(i, c):
        rows = rows_of(i)
        squares = jnp.zeros((tile, 1), F32)
        for j in range(nt):
            x = merged[j, rows, :].astype(F32)
            squares += jnp.sum(x * x, axis=1, keepdims=True)
        factor = lax.rsqrt(squares / depth + EPS)
        squares = jnp.zeros((tile, 1), F32)
        for j in range(nt):
            x = merged[j, rows, :].astype(F32)
            y = (toks[j, rows, :].astype(F32) + x * factor * merge_gain[j]).astype(BF16)
            toks[j, rows, :] = y
            y = y.astype(F32)
            squares += jnp.sum(y * y, axis=1, keepdims=True)
        factor = lax.rsqrt(squares / depth + EPS)
        for j in range(nt):
            y = toks[j, rows, :].astype(F32)
            nrm[rows, pl.ds(j * width, width)] = (y * factor * channel_gain[j]).astype(BF16)
        return c

    lax.fori_loop(0, tiles, first_tile, 0)
    first_out[...] = toks[t]
    ring_close(FEED)

    def feed_tile(i, c):
        rows = rows_of(i)
        x = nrm[rows, :]
        gate = jnp.dot(x, full_gate[...], preferred_element_type=F32)
        upward = jnp.dot(x, full_up[...], preferred_element_type=F32)
        hidden[rows, :] = (gate / (1.0 + jnp.exp(-gate)) * upward).astype(BF16)
        return c

    lax.fori_loop(0, tiles // 2, feed_tile, 0)
    pump(DOWN, 1)
    lax.fori_loop(tiles // 2, tiles, feed_tile, 0)
    pump(DOWN, 2)

    def down_copy(b):
        j = b // bps
        q = lax.rem(b, bps)
        o = lax.rem(j - t + nt, nt)
        return pltpu.make_async_remote_copy(
            src_ref=part.at[b], dst_ref=drecv.at[o - 1, q],
            send_sem=dn_send.at[b], recv_sem=dn_recv.at[o - 1, q],
            device_id={"tp": j}, device_id_type=MESH,
        )

    def down_block(k):
        b = owner(pos + k)
        part[b] = jnp.dot(hidden[...], full_down[b], preferred_element_type=F32).astype(BF16)

        @pl.when(b // bps != t)
        def _():
            down_copy(b).start()

    down_block(0)
    pumps(DOWN, 3, half)

    def down_step(s, c):
        for w in DOWN:
            for d in (0, 1):
                ring_arrive(w, d, s)
                ring_copy(w, d, s).wait_send()

                @pl.when(s < n - 2)
                def _():
                    ring_copy(w, d, s + 1).start()

        down_block(s + 1)

        @pl.when(s + 1 != n - 1 - s)
        def _():
            down_block(n - 1 - s)

        return c

    lax.fori_loop(half - 1, n - 1, down_step, 0)
    for o in offsets:
        for q in range(bps):
            got = drecv.at[o - 1, q]
            pltpu.make_async_remote_copy(
                src_ref=got, dst_ref=got, send_sem=dn_send.at[0], recv_sem=dn_recv.at[o - 1, q],
                device_id={"tp": peer(o)}, device_id_type=MESH,
            ).wait_recv()
    add_tile(drecv, down_out)
    for o in offsets:
        for q in range(bps):
            down_copy(peer(o) * bps + q).wait_send()


def finish(summed, residual, gain_row):
    floats = summed.astype(F32)
    columns = floats.shape[1]
    squares = lax.psum(jnp.sum(floats * floats, axis=1), "tp")
    factor = lax.rsqrt(squares / (columns * lax.axis_size("tp")) + EPS)
    own_gain = lax.dynamic_slice_in_dim(gain_row, lax.axis_index("tp") * columns, columns)
    return (residual.astype(F32) + floats * factor[:, None] * own_gain).astype(BF16)


def solution(mesh):
    n, nt = mesh.shape["fs"], mesh.shape["tp"]

    def shards(
        tokens, mixer_gain, conv_taps, outer_weight, inner_weight, value_weight, merge_weight,
        merge_gain, channel_gain, gate_weight, up_weight, down_weight, output_gain,
    ):
        length, width = tokens.shape
        blk, channels = outer_weight.shape
        units = gate_weight.shape[1]
        cols = merge_weight.shape[1]
        depth = width * nt
        bps = n // nt
        own_taps = lax.dynamic_slice_in_dim(
            conv_taps, lax.axis_index("tp") * channels, channels, 1
        ).astype(F32)

        def slabs(gain):
            return gain.reshape(nt, 1, width)

        vmem = pl.BlockSpec(memory_space=pltpu.VMEM)
        dma = pltpu.SemaphoreType.DMA
        down, first = pl.pallas_call(
            lambda *refs: layer_kernel(n, nt, *refs),
            out_shape=[jax.ShapeDtypeStruct((length, width), BF16)] * 2,
            in_specs=[vmem] * 12,
            out_specs=[vmem] * 2,
            scratch_shapes=[
                pltpu.VMEM((nt, length, width), BF16),
                pltpu.VMEM((length, depth), BF16),
                pltpu.VMEM((n * blk, channels), BF16),
                pltpu.VMEM((n * blk, channels), BF16),
                pltpu.VMEM((n * blk, channels), BF16),
                pltpu.VMEM((n, channels, cols), BF16),
                pltpu.VMEM((n * blk, units), BF16),
                pltpu.VMEM((n * blk, units), BF16),
                pltpu.VMEM((n, units, cols), BF16),
                pltpu.VMEM((length, channels), F32),
                pltpu.VMEM((length + 8, channels), F32),
                pltpu.VMEM((length, channels), BF16),
                pltpu.VMEM((n, length, cols), BF16),
                pltpu.VMEM((nt - 1, bps, length, cols), BF16),
                pltpu.VMEM((length, width), BF16),
                pltpu.VMEM((nt, length, width), BF16),
                pltpu.VMEM((length, units), BF16),
                pltpu.VMEM((nt - 1, bps, length, cols), BF16),
                dma((2, 8)),
                dma((2, 8, n - 1)),
                dma((nt - 1,)), dma((nt - 1,)),
                dma((nt - 1,)), dma((nt - 1,)),
                dma((nt - 1,)), dma((nt - 1,)),
                dma((n,)), dma((nt - 1, bps)),
            ],
            compiler_params=pltpu.CompilerParams(
                collective_id=0, has_side_effects=True, vmem_limit_bytes=67043328
            ),
        )(
            tokens, slabs(mixer_gain), own_taps, outer_weight, inner_weight, value_weight,
            merge_weight, slabs(merge_gain), slabs(channel_gain), gate_weight, up_weight,
            down_weight,
        )
        return finish(down, first, output_gain)

    return jax.shard_map(
        shards,
        mesh=mesh,
        in_specs=(
            P("fs", "tp"), P(), P(), P("fs", "tp"), P("fs", "tp"), P("fs", "tp"), P("tp", "fs"),
            P(), P(), P("fs", "tp"), P("fs", "tp"), P("tp", "fs"), P(),
        ),
        out_specs=P("fs", "tp"),
        check_vma=False,
    )
```

```python
import jax
import jax.numpy as jnp
from jax import lax
from jax.experimental import pallas as pl
from jax.experimental.pallas import tpu as pltpu
from jax.sharding import PartitionSpec as P

HEAD_DIM = 128
EPS = 1e-06
MESH = pl.DeviceIdType.MESH
F32 = jnp.float32
BF16 = jnp.bfloat16
MIX, FEED, DOWN = (0, 1, 2, 3), (4, 5), (6, 7)


def layer_kernel(
    n, nt, tokens, mixer_gain, conv_taps, outer_w, inner_w, value_w, merge_w, merge_gain,
    channel_gain, gate_w, up_w, down_w, output_gain,
    out,
    toks, nrm, full_outer, full_inner, full_value, full_merge, full_gate, full_up, full_down,
    outer_s, sig, mixed, part, mrecv, msum, merged, hidden, drecv, sq_own, sq_in,
    ring_send, ring_recv, tok_send, tok_recv, rs_send, rs_recv, ag_send, ag_recv, dn_send, dn_recv,
    sq_send, sq_recv,
):
    f, t = lax.axis_index("fs"), lax.axis_index("tp")
    half = n // 2
    odd = lax.rem(f, 2)
    pos = (1 - odd) * (f // 2) + odd * (n - 1 - f // 2)
    length, width = tokens.shape
    blk, channels = outer_w.shape
    cols = merge_w.shape[1]
    bps = n // nt
    depth = width * nt
    tile = min(256, length)
    tiles = length // tile

    def owner(p):
        q = lax.rem(p + 2 * n, n)
        high = q // half
        return (1 - high) * (2 * q) + high * (2 * (n - 1 - q) + 1)

    right, left = owner(pos + 1), owner(pos - 1)
    rowed = {0: (outer_w, full_outer), 1: (inner_w, full_inner), 2: (value_w, full_value),
             4: (gate_w, full_gate), 5: (up_w, full_up)}
    piece_m = channels // 2
    piece_d = down_w.shape[0] // 4

    def own_region(w, h):
        if w in rowed:
            return rowed[w][0].at[pl.ds(h * (blk // 2), blk // 2)]
        if w == 3:
            return merge_w.at[pl.ds(h * piece_m, piece_m)]
        return down_w.at[pl.ds((h * 2 + w - 6) * piece_d, piece_d)]

    def region(w, h, p):
        i = owner(p)
        if w in rowed:
            start = pl.multiple_of(i * blk + h * (blk // 2), blk // 2)
            return rowed[w][1].at[pl.ds(start, blk // 2)]
        if w == 3:
            return full_merge.at[i, pl.ds(h * piece_m, piece_m)]
        return full_down.at[i, pl.ds((h * 2 + w - 6) * piece_d, piece_d)]

    def ring_copy(w, h, d, s, first=False):
        dst = region(w, h, pos - s if d == 0 else pos + s)
        return pltpu.make_async_remote_copy(
            src_ref=own_region(w, h) if first else dst,
            dst_ref=dst,
            send_sem=ring_send.at[d, h, w],
            recv_sem=ring_recv.at[d, h, w, s],
            device_id={"fs": right if d == 0 else left},
            device_id_type=MESH,
        )

    def ring_arrive(w, h, d, s):
        got = region(w, h, pos - 1 - s if d == 0 else pos + 1 + s)
        pltpu.make_async_remote_copy(
            src_ref=got, dst_ref=got, send_sem=ring_send.at[d, h, w],
            recv_sem=ring_recv.at[d, h, w, s],
            device_id={"fs": right if d == 0 else left}, device_id_type=MESH,
        ).wait_recv()

    def pieces(ws):
        return [(w, h, d) for h in (0, 1) for w in ws for d in (0, 1)]

    def ring_open(ws):
        for w, h, d in pieces(ws):
            ring_copy(w, h, d, 0, True).start()

    def pump(ws, s, last=False):
        for w, h, d in pieces(ws):
            if last and h != d:
                continue
            ring_arrive(w, h, d, s - 1)
            ring_copy(w, h, d, s - 1).wait_send()
            ring_copy(w, h, d, s).start()
        for w, h, d in pieces(ws):
            if last and h != d:
                ring_arrive(w, h, d, s - 1)
                ring_copy(w, h, d, s - 1).wait_send()

    def pumps(ws, low, high):
        lax.fori_loop(low, high, lambda s, c: (pump(ws, s), c)[1], 0)

    def ring_close(ws):
        for w in ws:
            for d in (0, 1):
                ring_arrive(w, d, d, half - 1)
                ring_copy(w, d, d, half - 1).wait_send()

    def peer(o):
        return lax.rem(t + o, nt)

    def slab_copy(src, dst, send, recv, o):
        return pltpu.make_async_remote_copy(
            src_ref=src, dst_ref=dst, send_sem=send.at[o - 1], recv_sem=recv.at[o - 1],
            device_id={"tp": peer(o)}, device_id_type=MESH,
        )

    offsets = range(1, nt)
    partner = t + 1 - 2 * lax.rem(t, 2)
    strides = range(2, nt, 2)

    def hop(src, dst, send, recv, i, to):
        return pltpu.make_async_remote_copy(
            src_ref=src, dst_ref=dst, send_sem=send.at[i], recv_sem=recv.at[i],
            device_id={"tp": to}, device_id_type=MESH,
        )

    def gather_open(own, held, send, recv):
        for o in strides:
            hop(own, held.at[t], send, recv, o - 1, peer(o)).start()
        hop(own, held.at[t], send, recv, 0, partner).start()

    def gather_relay(own, held, send, recv):
        for o in strides:
            slab = held.at[peer(nt - o)]
            hop(own, slab, send, recv, o - 1, peer(o)).wait()
            hop(slab, slab, send, recv, o, partner).start()

    def gather_close(own, held, send, recv):
        hop(own, held.at[partner], send, recv, 0, partner).wait()
        for o in strides:
            slab = held.at[lax.rem(partner + nt - o, nt)]
            hop(held.at[peer(nt - o)], slab, send, recv, o, partner).wait()

    tok_args = (tokens, toks, tok_send, tok_recv)
    sum_args = (msum, merged, ag_send, ag_recv)

    barrier = pltpu.get_barrier_semaphore()
    for to in ({"fs": left}, {"fs": right}) + tuple({"tp": peer(o)} for o in offsets):
        pl.semaphore_signal(barrier, inc=1, device_id=to, device_id_type=MESH)
    pl.semaphore_wait(barrier, 2 + nt - 1)

    ring_open(MIX)
    gather_open(*tok_args)

    own_rows = pl.ds(pl.multiple_of(f * blk, blk), blk)
    for source, full in rowed.values():
        full[own_rows, :] = source[...]
    full_merge[f] = merge_w[...]
    full_down[f] = down_w[...]
    toks[t] = tokens[...]
    sig[pl.ds(0, 8), :] = jnp.zeros((8, channels), F32)

    pumps(MIX, 1, half - 1)
    gather_relay(*tok_args)
    pump(MIX, half - 1, True)
    ring_open(FEED)
    gather_close(*tok_args)
    taps = conv_taps[:, pl.ds(pl.multiple_of(t * channels, channels), channels)].astype(F32)

    def rows_of(i):
        return pl.ds(pl.multiple_of(i * tile, tile), tile)

    def norm_tile(i, c):
        rows = rows_of(i)
        squares = jnp.zeros((tile, 1), F32)
        for j in range(nt):
            x = toks[j, rows, :].astype(F32)
            squares += jnp.sum(x * x, axis=1, keepdims=True)
        factor = lax.rsqrt(squares / depth + EPS)
        for j in range(nt):
            x = toks[j, rows, :].astype(F32)
            nrm[rows, pl.ds(j * width, width)] = (x * factor * mixer_gain[j]).astype(BF16)
        return c

    lax.fori_loop(0, tiles, norm_tile, 0)
    ring_close(MIX)

    def project(i, c):
        rows = rows_of(i)
        x = nrm[rows, :]
        outer_s[rows, :] = jnp.dot(x, full_outer[...], preferred_element_type=F32)
        inner = jnp.dot(x, full_inner[...], preferred_element_type=F32)
        value = jnp.dot(x, full_value[...], preferred_element_type=F32)
        sig[pl.ds(pl.multiple_of(i * tile + 8, 8), tile), :] = inner * value
        return c

    lax.fori_loop(0, tiles, project, 0)
    for i in range(tiles):
        r = i * tile
        conv = (
            taps[0:1, :] * sig[r + 6 : r + 6 + tile, :]
            + taps[1:2, :] * sig[r + 7 : r + 7 + tile, :]
            + taps[2:3, :] * sig[r + 8 : r + 8 + tile, :]
        )
        gated = outer_s[r : r + tile, :] * conv
        for h in range(channels // HEAD_DIM):
            g = gated[:, h * HEAD_DIM : (h + 1) * HEAD_DIM]
            level = lax.rsqrt(jnp.mean(g * g, axis=1, keepdims=True) + EPS)
            mixed[r : r + tile, h * HEAD_DIM : (h + 1) * HEAD_DIM] = (g * level).astype(BF16)

    def merge_block(b, c):
        part[b] = jnp.dot(mixed[...], full_merge[b], preferred_element_type=F32).astype(BF16)
        return c

    lax.fori_loop(0, n, merge_block, 0)

    def part_slab(j):
        return part.at[pl.ds(j * bps, bps)]

    for o in offsets:
        slab_copy(part_slab(peer(o)), mrecv.at[o - 1], rs_send, rs_recv, o).start()
    pumps(FEED, 1, half - 1)
    for o in offsets:
        slab_copy(part_slab(peer(o)), mrecv.at[o - 1], rs_send, rs_recv, o).wait()

    def add_tile(received, target):
        def body(i, c):
            rows = rows_of(i)
            for q in range(bps):
                total = part[t * bps + q, rows, :].astype(F32)
                for o in offsets:
                    total += received[o - 1, q, rows, :].astype(F32)
                target[rows, pl.ds(q * cols, cols)] = total.astype(BF16)
            return c

        lax.fori_loop(0, tiles, body, 0)

    add_tile(mrecv, msum)
    gather_open(*sum_args)
    merged[t] = msum[...]
    pump(FEED, half - 1, True)
    ring_open(DOWN)
    gather_relay(*sum_args)
    gather_close(*sum_args)

    def first_tile(i, c):
        rows = rows_of(i)
        squares = jnp.zeros((tile, 1), F32)
        for j in range(nt):
            x = merged[j, rows, :].astype(F32)
            squares += jnp.sum(x * x, axis=1, keepdims=True)
        factor = lax.rsqrt(squares / depth + EPS)
        squares = jnp.zeros((tile, 1), F32)
        for j in range(nt):
            x = merged[j, rows, :].astype(F32)
            y = (toks[j, rows, :].astype(F32) + x * factor * merge_gain[j]).astype(BF16)
            toks[j, rows, :] = y
            y = y.astype(F32)
            squares += jnp.sum(y * y, axis=1, keepdims=True)
        factor = lax.rsqrt(squares / depth + EPS)
        for j in range(nt):
            y = toks[j, rows, :].astype(F32)
            nrm[rows, pl.ds(j * width, width)] = (y * factor * channel_gain[j]).astype(BF16)
        return c

    lax.fori_loop(0, tiles, first_tile, 0)
    ring_close(FEED)

    def feed_tile(i, c):
        rows = rows_of(i)
        x = nrm[rows, :]
        gate = jnp.dot(x, full_gate[...], preferred_element_type=F32)
        upward = jnp.dot(x, full_up[...], preferred_element_type=F32)
        hidden[rows, :] = (gate / (1.0 + jnp.exp(-gate)) * upward).astype(BF16)
        return c

    lax.fori_loop(0, tiles * 3 // 4, feed_tile, 0)
    pump(DOWN, 1)
    lax.fori_loop(tiles * 3 // 4, tiles, feed_tile, 0)

    def down_copy(b):
        j = b // bps
        q = lax.rem(b, bps)
        o = lax.rem(j - t + nt, nt)
        return pltpu.make_async_remote_copy(
            src_ref=part.at[b], dst_ref=drecv.at[o - 1, q],
            send_sem=dn_send.at[b], recv_sem=dn_recv.at[o - 1, q],
            device_id={"tp": j}, device_id_type=MESH,
        )

    def down_block(k):
        b = owner(pos + k)
        part[b] = jnp.dot(hidden[...], full_down[b], preferred_element_type=F32).astype(BF16)

        @pl.when(b // bps != t)
        def _():
            down_copy(b).start()

    def down_pair(s):
        lax.fori_loop(0, 2, lambda i, c: (down_block(s - 2 * s * i), c)[1], 0)

    def down_step(s, c):
        pump(DOWN, s)
        down_pair(s)
        return c

    down_block(0)
    down_pair(1)
    lax.fori_loop(2, half - 1, down_step, 0)
    pump(DOWN, half - 1, True)
    down_pair(half - 1)
    ring_close(DOWN)
    down_block(half)
    for o in offsets:
        for q in range(bps):
            got = drecv.at[o - 1, q]
            pltpu.make_async_remote_copy(
                src_ref=got, dst_ref=got, send_sem=dn_send.at[0], recv_sem=dn_recv.at[o - 1, q],
                device_id={"tp": peer(o)}, device_id_type=MESH,
            ).wait_recv()
    add_tile(drecv, msum)

    def square_tile(i, c):
        rows = rows_of(i)
        x = msum[rows, :].astype(F32)
        sq_own[:, rows] = lax.dot_general(
            jnp.ones((8, width), F32), x * x, (((1,), (1,)), ((), ())),
            precision=lax.Precision.HIGHEST, preferred_element_type=F32,
        )
        return c

    lax.fori_loop(0, tiles, square_tile, 0)
    for o in offsets:
        slab_copy(sq_own, sq_in.at[o - 1], sq_send, sq_recv, o).start()
    for o in offsets:
        for q in range(bps):
            down_copy(peer(o) * bps + q).wait_send()
    for o in offsets:
        slab_copy(sq_own, sq_in.at[o - 1], sq_send, sq_recv, o).wait()

    def last_tile(i, c):
        rows = rows_of(i)
        squares = sq_own[:, rows]
        for o in offsets:
            squares += sq_in[o - 1, :, rows]
        factor = lax.rsqrt(jnp.transpose(squares)[:, 0:1] / depth + EPS)
        y = toks[t, rows, :].astype(F32) + msum[rows, :].astype(F32) * factor * output_gain[t]
        out[rows, :] = y.astype(BF16)
        return c

    lax.fori_loop(0, tiles, last_tile, 0)


def solution(mesh):
    n, nt = mesh.shape["fs"], mesh.shape["tp"]

    def shards(
        tokens, mixer_gain, conv_taps, outer_weight, inner_weight, value_weight, merge_weight,
        merge_gain, channel_gain, gate_weight, up_weight, down_weight, output_gain,
    ):
        length, width = tokens.shape
        blk, channels = outer_weight.shape
        units = gate_weight.shape[1]
        cols = merge_weight.shape[1]
        depth = width * nt
        bps = n // nt
        def slabs(gain):
            return gain.reshape(nt, 1, width)

        vmem = pl.BlockSpec(memory_space=pltpu.VMEM)
        dma = pltpu.SemaphoreType.DMA
        return pl.pallas_call(
            lambda *refs: layer_kernel(n, nt, *refs),
            out_shape=jax.ShapeDtypeStruct((length, width), BF16),
            in_specs=[vmem] * 13,
            out_specs=vmem,
            scratch_shapes=[
                pltpu.VMEM((nt, length, width), BF16),
                pltpu.VMEM((length, depth), BF16),
                pltpu.VMEM((n * blk, channels), BF16),
                pltpu.VMEM((n * blk, channels), BF16),
                pltpu.VMEM((n * blk, channels), BF16),
                pltpu.VMEM((n, channels, cols), BF16),
                pltpu.VMEM((n * blk, units), BF16),
                pltpu.VMEM((n * blk, units), BF16),
                pltpu.VMEM((n, units, cols), BF16),
                pltpu.VMEM((length, channels), F32),
                pltpu.VMEM((length + 8, channels), F32),
                pltpu.VMEM((length, channels), BF16),
                pltpu.VMEM((n, length, cols), BF16),
                pltpu.VMEM((nt - 1, bps, length, cols), BF16),
                pltpu.VMEM((length, width), BF16),
                pltpu.VMEM((nt, length, width), BF16),
                pltpu.VMEM((length, units), BF16),
                pltpu.VMEM((nt - 1, bps, length, cols), BF16),
                pltpu.VMEM((8, length), F32),
                pltpu.VMEM((nt - 1, 8, length), F32),
                dma((2, 2, 8)),
                dma((2, 2, 8, n // 2)),
                dma((nt - 1,)), dma((nt - 1,)),
                dma((nt - 1,)), dma((nt - 1,)),
                dma((nt - 1,)), dma((nt - 1,)),
                dma((n,)), dma((nt - 1, bps)),
                dma((nt - 1,)), dma((nt - 1,)),
            ],
            compiler_params=pltpu.CompilerParams(
                collective_id=0, has_side_effects=True, vmem_limit_bytes=67043328
            ),
        )(
            tokens, slabs(mixer_gain), conv_taps, outer_weight, inner_weight, value_weight,
            merge_weight, slabs(merge_gain), slabs(channel_gain), gate_weight, up_weight,
            down_weight, slabs(output_gain),
        )

    return jax.shard_map(
        shards,
        mesh=mesh,
        in_specs=(
            P("fs", "tp"), P(), P(), P("fs", "tp"), P("fs", "tp"), P("fs", "tp"), P("tp", "fs"),
            P(), P(), P("fs", "tp"), P("fs", "tp"), P("tp", "fs"), P(),
        ),
        out_specs=P("fs", "tp"),
        check_vma=False,
    )
```

```python
import jax
import jax.numpy as jnp
from jax import lax
from jax.experimental import pallas as pl
from jax.experimental.pallas import tpu as pltpu
from jax.sharding import PartitionSpec as P

HEAD_DIM = 128
EPS = 1e-06
MESH = pl.DeviceIdType.MESH
F32 = jnp.float32
BF16 = jnp.bfloat16
MIX, FEED, DOWN = (0, 1, 2, 3), (4, 5), (6, 7)


def layer_kernel(
    n, nt, tokens, mixer_gain, conv_taps, outer_w, inner_w, value_w, merge_w, merge_gain,
    channel_gain, gate_w, up_w, down_w, output_gain,
    out,
    toks, nrm, full_outer, full_inner, full_value, full_merge, full_gate, full_up, full_down,
    outer_s, sig, mixed, part, mrecv, msum, merged, hidden, drecv, sq_own, sq_in,
    ring_send, ring_recv, tok_send, tok_recv, rs_send, rs_recv, ag_send, ag_recv, dn_send, dn_recv,
    sq_send, sq_recv,
):
    f, t = lax.axis_index("fs"), lax.axis_index("tp")
    half = n // 2
    odd = lax.rem(f, 2)
    pos = (1 - odd) * (f // 2) + odd * (n - 1 - f // 2)
    length, width = tokens.shape
    blk, channels = outer_w.shape
    cols = merge_w.shape[1]
    bps = n // nt
    depth = width * nt
    tile = min(256, length)
    tiles = length // tile

    def owner(p):
        q = lax.rem(p + 2 * n, n)
        high = q // half
        return (1 - high) * (2 * q) + high * (2 * (n - 1 - q) + 1)

    right, left = owner(pos + 1), owner(pos - 1)
    rowed = {0: (outer_w, full_outer), 1: (inner_w, full_inner), 2: (value_w, full_value),
             4: (gate_w, full_gate), 5: (up_w, full_up)}
    piece_m = channels // 2
    piece_d = down_w.shape[0] // 4

    def own_region(w, h):
        if w in rowed:
            return rowed[w][0].at[pl.ds(h * (blk // 2), blk // 2)]
        if w == 3:
            return merge_w.at[pl.ds(h * piece_m, piece_m)]
        return down_w.at[pl.ds((h * 2 + w - 6) * piece_d, piece_d)]

    def region(w, h, p):
        i = owner(p)
        if w in rowed:
            start = pl.multiple_of(i * blk + h * (blk // 2), blk // 2)
            return rowed[w][1].at[pl.ds(start, blk // 2)]
        if w == 3:
            return full_merge.at[i, pl.ds(h * piece_m, piece_m)]
        return full_down.at[i, pl.ds((h * 2 + w - 6) * piece_d, piece_d)]

    def ring_copy(w, h, d, s, first=False):
        dst = region(w, h, pos - s if d == 0 else pos + s)
        return pltpu.make_async_remote_copy(
            src_ref=own_region(w, h) if first else dst,
            dst_ref=dst,
            send_sem=ring_send.at[d, h, w],
            recv_sem=ring_recv.at[d, h, w, s],
            device_id={"fs": right if d == 0 else left},
            device_id_type=MESH,
        )

    def ring_arrive(w, h, d, s):
        got = region(w, h, pos - 1 - s if d == 0 else pos + 1 + s)
        pltpu.make_async_remote_copy(
            src_ref=got, dst_ref=got, send_sem=ring_send.at[d, h, w],
            recv_sem=ring_recv.at[d, h, w, s],
            device_id={"fs": right if d == 0 else left}, device_id_type=MESH,
        ).wait_recv()

    def pieces(ws):
        return [(w, (i + d) % 2, d) for i in (0, 1) for w in ws for d in (0, 1)]

    def ring_open(ws):
        for w, h, d in pieces(ws):
            ring_copy(w, h, d, 0, True).start()

    def pump(ws, s, last=False):
        for w, h, d in pieces(ws):
            if last and h != d:
                continue
            ring_arrive(w, h, d, s - 1)
            ring_copy(w, h, d, s - 1).wait_send()
            ring_copy(w, h, d, s).start()
        for w, h, d in pieces(ws):
            if last and h != d:
                ring_arrive(w, h, d, s - 1)
                ring_copy(w, h, d, s - 1).wait_send()

    def pumps(ws, low, high):
        lax.fori_loop(low, high, lambda s, c: (pump(ws, s), c)[1], 0)

    def ring_close(ws):
        for w in ws:
            for d in (0, 1):
                ring_arrive(w, d, d, half - 1)
                ring_copy(w, d, d, half - 1).wait_send()

    def peer(o):
        return lax.rem(t + o, nt)

    def slab_copy(src, dst, send, recv, o):
        return pltpu.make_async_remote_copy(
            src_ref=src, dst_ref=dst, send_sem=send.at[o - 1], recv_sem=recv.at[o - 1],
            device_id={"tp": peer(o)}, device_id_type=MESH,
        )

    offsets = range(1, nt)
    partner = t + 1 - 2 * lax.rem(t, 2)
    strides = range(2, nt, 2)

    def hop(src, dst, send, recv, i, to):
        return pltpu.make_async_remote_copy(
            src_ref=src, dst_ref=dst, send_sem=send.at[i], recv_sem=recv.at[i],
            device_id={"tp": to}, device_id_type=MESH,
        )

    def gather_open(own, held, send, recv):
        for o in strides:
            hop(own, held.at[t], send, recv, o - 1, peer(o)).start()
        hop(own, held.at[t], send, recv, 0, partner).start()

    def gather_relay(own, held, send, recv):
        for o in strides:
            slab = held.at[peer(nt - o)]
            hop(own, slab, send, recv, o - 1, peer(o)).wait()
            hop(slab, slab, send, recv, o, partner).start()

    def gather_close(own, held, send, recv):
        hop(own, held.at[partner], send, recv, 0, partner).wait()
        for o in strides:
            slab = held.at[lax.rem(partner + nt - o, nt)]
            hop(held.at[peer(nt - o)], slab, send, recv, o, partner).wait()

    tok_args = (tokens, toks, tok_send, tok_recv)
    sum_args = (msum, merged, ag_send, ag_recv)

    barrier = pltpu.get_barrier_semaphore()
    for to in ({"fs": left}, {"fs": right}) + tuple({"tp": peer(o)} for o in offsets):
        pl.semaphore_signal(barrier, inc=1, device_id=to, device_id_type=MESH)
    pl.semaphore_wait(barrier, 2 + nt - 1)

    ring_open(MIX)
    gather_open(*tok_args)

    own_rows = pl.ds(pl.multiple_of(f * blk, blk), blk)
    for source, full in rowed.values():
        full[own_rows, :] = source[...]
    full_merge[f] = merge_w[...]
    full_down[f] = down_w[...]
    toks[t] = tokens[...]
    sig[pl.ds(0, 8), :] = jnp.zeros((8, channels), F32)

    pumps(MIX, 1, half - 1)
    gather_relay(*tok_args)
    pump(MIX, half - 1, True)
    ring_open(FEED)
    gather_close(*tok_args)
    taps = conv_taps[:, pl.ds(pl.multiple_of(t * channels, channels), channels)].astype(F32)

    def rows_of(i):
        return pl.ds(pl.multiple_of(i * tile, tile), tile)

    def norm_tile(i, c):
        rows = rows_of(i)
        squares = jnp.zeros((tile, 1), F32)
        for j in range(nt):
            x = toks[j, rows, :].astype(F32)
            squares += jnp.sum(x * x, axis=1, keepdims=True)
        factor = lax.rsqrt(squares / depth + EPS)
        for j in range(nt):
            x = toks[j, rows, :].astype(F32)
            nrm[rows, pl.ds(j * width, width)] = (x * factor * mixer_gain[j]).astype(BF16)
        return c

    lax.fori_loop(0, tiles, norm_tile, 0)
    ring_close(MIX)

    def project(i, c):
        rows = rows_of(i)
        x = nrm[rows, :]
        outer_s[rows, :] = jnp.dot(x, full_outer[...], preferred_element_type=F32)
        inner = jnp.dot(x, full_inner[...], preferred_element_type=F32)
        value = jnp.dot(x, full_value[...], preferred_element_type=F32)
        sig[pl.ds(pl.multiple_of(i * tile + 8, 8), tile), :] = inner * value
        return c

    lax.fori_loop(0, tiles, project, 0)
    for i in range(tiles):
        r = i * tile
        conv = (
            taps[0:1, :] * sig[r + 6 : r + 6 + tile, :]
            + taps[1:2, :] * sig[r + 7 : r + 7 + tile, :]
            + taps[2:3, :] * sig[r + 8 : r + 8 + tile, :]
        )
        gated = outer_s[r : r + tile, :] * conv
        for h in range(channels // HEAD_DIM):
            g = gated[:, h * HEAD_DIM : (h + 1) * HEAD_DIM]
            level = lax.rsqrt(jnp.mean(g * g, axis=1, keepdims=True) + EPS)
            mixed[r : r + tile, h * HEAD_DIM : (h + 1) * HEAD_DIM] = (g * level).astype(BF16)

    def merge_block(b, c):
        part[b] = jnp.dot(mixed[...], full_merge[b], preferred_element_type=F32).astype(BF16)
        return c

    lax.fori_loop(0, n, merge_block, 0)

    def part_slab(j):
        return part.at[pl.ds(j * bps, bps)]

    for o in offsets:
        slab_copy(part_slab(peer(o)), mrecv.at[o - 1], rs_send, rs_recv, o).start()
    pumps(FEED, 1, half - 1)
    for o in offsets:
        slab_copy(part_slab(peer(o)), mrecv.at[o - 1], rs_send, rs_recv, o).wait()

    def add_tile(received, target):
        def body(i, c):
            rows = rows_of(i)
            for q in range(bps):
                total = part[t * bps + q, rows, :].astype(F32)
                for o in offsets:
                    total += received[o - 1, q, rows, :].astype(F32)
                target[rows, pl.ds(q * cols, cols)] = total.astype(BF16)
            return c

        lax.fori_loop(0, tiles, body, 0)

    add_tile(mrecv, msum)
    gather_open(*sum_args)
    merged[t] = msum[...]
    pump(FEED, half - 1, True)
    ring_open(DOWN)
    gather_relay(*sum_args)
    gather_close(*sum_args)

    def first_tile(i, c):
        rows = rows_of(i)
        squares = jnp.zeros((tile, 1), F32)
        for j in range(nt):
            x = merged[j, rows, :].astype(F32)
            squares += jnp.sum(x * x, axis=1, keepdims=True)
        factor = lax.rsqrt(squares / depth + EPS)
        squares = jnp.zeros((tile, 1), F32)
        for j in range(nt):
            x = merged[j, rows, :].astype(F32)
            y = (toks[j, rows, :].astype(F32) + x * factor * merge_gain[j]).astype(BF16)
            toks[j, rows, :] = y
            y = y.astype(F32)
            squares += jnp.sum(y * y, axis=1, keepdims=True)
        factor = lax.rsqrt(squares / depth + EPS)
        for j in range(nt):
            y = toks[j, rows, :].astype(F32)
            nrm[rows, pl.ds(j * width, width)] = (y * factor * channel_gain[j]).astype(BF16)
        return c

    lax.fori_loop(0, tiles, first_tile, 0)
    ring_close(FEED)

    def feed_tile(i, c):
        rows = rows_of(i)
        x = nrm[rows, :]
        gate = jnp.dot(x, full_gate[...], preferred_element_type=F32)
        upward = jnp.dot(x, full_up[...], preferred_element_type=F32)
        hidden[rows, :] = (gate / (1.0 + jnp.exp(-gate)) * upward).astype(BF16)
        return c

    lax.fori_loop(0, tiles * 3 // 4, feed_tile, 0)
    pump(DOWN, 1)
    lax.fori_loop(tiles * 3 // 4, tiles, feed_tile, 0)

    def down_copy(b):
        j = b // bps
        q = lax.rem(b, bps)
        o = lax.rem(j - t + nt, nt)
        return pltpu.make_async_remote_copy(
            src_ref=part.at[b], dst_ref=drecv.at[o - 1, q],
            send_sem=dn_send.at[b], recv_sem=dn_recv.at[o - 1, q],
            device_id={"tp": j}, device_id_type=MESH,
        )

    def down_block(k):
        b = owner(pos + k)
        part[b] = jnp.dot(hidden[...], full_down[b], preferred_element_type=F32).astype(BF16)

        @pl.when(b // bps != t)
        def _():
            down_copy(b).start()

    def down_pair(s):
        lax.fori_loop(0, 2, lambda i, c: (down_block(s - 2 * s * i), c)[1], 0)

    def down_step(s, c):
        pump(DOWN, s)
        down_pair(s)
        return c

    down_block(0)
    down_pair(1)
    lax.fori_loop(2, half - 1, down_step, 0)
    pump(DOWN, half - 1, True)
    down_pair(half - 1)
    ring_close(DOWN)
    down_block(half)
    for o in offsets:
        for q in range(bps):
            got = drecv.at[o - 1, q]
            pltpu.make_async_remote_copy(
                src_ref=got, dst_ref=got, send_sem=dn_send.at[0], recv_sem=dn_recv.at[o - 1, q],
                device_id={"tp": peer(o)}, device_id_type=MESH,
            ).wait_recv()
    add_tile(drecv, msum)

    def square_tile(i, c):
        rows = rows_of(i)
        x = msum[rows, :].astype(F32)
        sq_own[:, rows] = lax.dot_general(
            jnp.ones((8, width), F32), x * x, (((1,), (1,)), ((), ())),
            precision=lax.Precision.HIGHEST, preferred_element_type=F32,
        )
        return c

    lax.fori_loop(0, tiles, square_tile, 0)
    for o in offsets:
        slab_copy(sq_own, sq_in.at[o - 1], sq_send, sq_recv, o).start()
    for o in offsets:
        for q in range(bps):
            down_copy(peer(o) * bps + q).wait_send()
    for o in offsets:
        slab_copy(sq_own, sq_in.at[o - 1], sq_send, sq_recv, o).wait()

    def last_tile(i, c):
        rows = rows_of(i)
        squares = sq_own[:, rows]
        for o in offsets:
            squares += sq_in[o - 1, :, rows]
        factor = lax.rsqrt(jnp.transpose(squares)[:, 0:1] / depth + EPS)
        y = toks[t, rows, :].astype(F32) + msum[rows, :].astype(F32) * factor * output_gain[t]
        out[rows, :] = y.astype(BF16)
        return c

    lax.fori_loop(0, tiles, last_tile, 0)


def solution(mesh):
    n, nt = mesh.shape["fs"], mesh.shape["tp"]

    def shards(
        tokens, mixer_gain, conv_taps, outer_weight, inner_weight, value_weight, merge_weight,
        merge_gain, channel_gain, gate_weight, up_weight, down_weight, output_gain,
    ):
        length, width = tokens.shape
        blk, channels = outer_weight.shape
        units = gate_weight.shape[1]
        cols = merge_weight.shape[1]
        depth = width * nt
        bps = n // nt
        def slabs(gain):
            return gain.reshape(nt, 1, width)

        vmem = pl.BlockSpec(memory_space=pltpu.VMEM)
        dma = pltpu.SemaphoreType.DMA
        return pl.pallas_call(
            lambda *refs: layer_kernel(n, nt, *refs),
            out_shape=jax.ShapeDtypeStruct((length, width), BF16),
            in_specs=[vmem] * 13,
            out_specs=vmem,
            scratch_shapes=[
                pltpu.VMEM((nt, length, width), BF16),
                pltpu.VMEM((length, depth), BF16),
                pltpu.VMEM((n * blk, channels), BF16),
                pltpu.VMEM((n * blk, channels), BF16),
                pltpu.VMEM((n * blk, channels), BF16),
                pltpu.VMEM((n, channels, cols), BF16),
                pltpu.VMEM((n * blk, units), BF16),
                pltpu.VMEM((n * blk, units), BF16),
                pltpu.VMEM((n, units, cols), BF16),
                pltpu.VMEM((length, channels), F32),
                pltpu.VMEM((length + 8, channels), F32),
                pltpu.VMEM((length, channels), BF16),
                pltpu.VMEM((n, length, cols), BF16),
                pltpu.VMEM((nt - 1, bps, length, cols), BF16),
                pltpu.VMEM((length, width), BF16),
                pltpu.VMEM((nt, length, width), BF16),
                pltpu.VMEM((length, units), BF16),
                pltpu.VMEM((nt - 1, bps, length, cols), BF16),
                pltpu.VMEM((8, length), F32),
                pltpu.VMEM((nt - 1, 8, length), F32),
                dma((2, 2, 8)),
                dma((2, 2, 8, n // 2)),
                dma((nt - 1,)), dma((nt - 1,)),
                dma((nt - 1,)), dma((nt - 1,)),
                dma((nt - 1,)), dma((nt - 1,)),
                dma((n,)), dma((nt - 1, bps)),
                dma((nt - 1,)), dma((nt - 1,)),
            ],
            compiler_params=pltpu.CompilerParams(
                collective_id=0, has_side_effects=True, vmem_limit_bytes=67043328
            ),
        )(
            tokens, slabs(mixer_gain), conv_taps, outer_weight, inner_weight, value_weight,
            merge_weight, slabs(merge_gain), slabs(channel_gain), gate_weight, up_weight,
            down_weight, slabs(output_gain),
        )

    return jax.shard_map(
        shards,
        mesh=mesh,
        in_specs=(
            P("fs", "tp"), P(), P(), P("fs", "tp"), P("fs", "tp"), P("fs", "tp"), P("tp", "fs"),
            P(), P(), P("fs", "tp"), P("fs", "tp"), P("tp", "fs"), P(),
        ),
        out_specs=P("fs", "tp"),
        check_vma=False,
    )
```
